128 devices in a mesh: fs: 32 (over z, y, core), tp: 4 (over x).
Axes of the slice: x: 4, y: 4, z: 4, core: 2. Of those that a mesh axis runs over, the one named last changes fastest.
Arguments:
- tokens: bfloat16 [24576, 2048], P('fs'), may hold values from -6 to 6
- norm_gain: float32 [2048], P('fs'), may hold values from 0.1 to 1.9
- gate_weight: float32 [2048, 5632], P('fs', 'tp'), may hold values from -0.125 to 0.125
- up_weight: float32 [2048, 5632], P('fs', 'tp'), may hold values from -0.125 to 0.125
- down_weight: float32 [5632, 2048], P('fs', 'tp'), may hold values from -0.078125 to 0.078125
Outputs:
- gate_out: bfloat16 [2048, 5632], P(None, 'tp')
- up_out: bfloat16 [2048, 5632], P(None, 'tp')
- down_out: bfloat16 [5632, 2048], P('tp')
- mixed: bfloat16 [24576, 2048], P('fs', 'tp')
The draws below stay inside these ranges and needn't reach their ends.
All inputs are finite; a program needn't handle non-finite values.
Results may differ from the reference program's by a relative error of at most 0.0095.
Values may be sent and summed in bfloat16 or wider, within the bound.
A program may use at most 128 MiB of HBM per device.

```python
import jax
import jax.numpy as jnp
from jax import lax

D = 2048
FF = 5632
TOKENS = 24576
N_TP = 4


def level_of(stream_key, dims, cuts, least, largest):
    gain, own = 1.0, jax.random.fold_in(stream_key, 6)
    for dim, blocks in cuts:
        heights = jnp.exp(jax.random.uniform(jax.random.fold_in(own, dim), (blocks,), jnp.float32, least / len(cuts), largest / len(cuts)))
        gain = gain * jnp.repeat(heights, dims[dim] // blocks).reshape([-1 if axis == dim else 1 for axis in range(len(dims))])
    return gain


def centred(rng, dims, width, reach, cuts=(), kind=jnp.bfloat16):
    result = width * jax.random.normal(rng, dims, jnp.float32)
    if cuts:
        result = result * level_of(rng, dims, cuts, -0.22, 0.18)
    return jnp.clip(result, -reach, reach).astype(kind)


def setup_inputs(seed: int = 0) -> dict:
    splits = jax.random.split(jax.random.key(seed), 6)
    return {
        "tokens": centred(splits[0], (TOKENS, D), 1.0, 6.0, ((0, 32),)),
        "norm_gain": jnp.clip(1.0 + 0.18 * jax.random.normal(splits[1], (D,), jnp.float32), 0.1, 1.9),
        "gate_weight": centred(splits[2], (D, FF), D ** -0.5, 0.125, ((0, 32), (1, 4)), jnp.float32),
        "up_weight": centred(splits[3], (D, FF), D ** -0.5, 0.125, ((0, 32), (1, 4)), jnp.float32),
        "down_weight": centred(splits[4], (FF, D), FF ** -0.5, 0.078125, ((0, 32), (1, 4)), jnp.float32),
    }


eps_norm = 1e-06

def reference(tokens, norm_gain, gate_weight, up_weight, down_weight):
    gain_column = norm_gain[:, None]
    gate_out = (gate_weight * gain_column).astype(jnp.bfloat16)
    up_out = (up_weight * gain_column).astype(jnp.bfloat16)
    down_out = down_weight.astype(jnp.bfloat16)
    rows_float = tokens.astype(jnp.float32)
    normed = (rows_float * lax.rsqrt(lax.optimization_barrier(jnp.mean(rows_float * rows_float, axis=-1, keepdims=True)) + eps_norm)).astype(jnp.bfloat16)
    gate_act = jnp.dot(normed, gate_out, preferred_element_type=jnp.float32)
    up_act = jnp.dot(normed, up_out, preferred_element_type=jnp.float32)
    hidden = (jax.nn.silu(gate_act) * up_act).astype(jnp.bfloat16)
    block_rows = FF // N_TP
    total = jnp.zeros((tokens.shape[0], D), jnp.float32)
    for index in range(N_TP):
        lower = index * block_rows
        share = jnp.dot(hidden[:, lower:lower + block_rows], down_out[lower:lower + block_rows, :], preferred_element_type=jnp.float32).astype(jnp.bfloat16)
        total = total + share.astype(jnp.float32)
    mixed = total.astype(jnp.bfloat16)
    return (gate_out, up_out, down_out, mixed)
```

```python
import jax
import jax.numpy as jnp
from jax import lax
from jax.experimental import pallas as pl
from jax.experimental.pallas import tpu as pltpu
from jax.sharding import PartitionSpec as P

MESH = pl.DeviceIdType.MESH
bf16, f32 = jnp.bfloat16, jnp.float32
eps_norm = 1e-06
RING = 4
CHUNKS = ((0, 384), (384, 384), (768, 384), (1152, 256))
NCH = len(CHUNKS)
PIECE = 256
OFFS = ((2, 0), (2, 1), (1, 0), (3, 0), (1, 1), (3, 1), (0, 0), (0, 1))
NP = len(OFFS)
TILE = 256


def ring(v, k):
    return lax.rem(v + k, RING)


def kernel(tok, gain, gw, uw, dw, W, Dn, mixed, X, H, gs, us, ds, dst, gv, S2, S1, R2, R1,
           in_sem, p1s, p1r, p2s, p2r, sbs, sbr, d0s, d0r, d1s, d1r, d2s, d2r, dbs, dbr, rss, rsr):
    x = lax.axis_index("tp")
    f = lax.axis_index("fs")
    c = lax.rem(f, 2)
    y = lax.rem(lax.div(f, 2), RING)
    z = lax.div(f, 2 * RING)
    rows, half = gs.shape[0], gs.shape[0] // 2
    drows, dcols = ds.shape
    dcut = 96

    def at(zz, yy, cc):
        return {"fs": (zz * RING + yy) * 2 + cc}

    zp, zm, yp, ym = ring(z, 1), ring(z, 3), ring(y, 1), ring(y, 3)
    near = ((at(zp, y, c), at(zm, y, c)), (at(z, yp, c), at(z, ym, c)))
    sibling = at(z, y, 1 - c)
    xnear = ({"tp": ring(x, 1)}, {"tp": ring(x, 3)})

    drain = []

    def copy(src, dst, ss, rs, dev):
        return pltpu.make_async_remote_copy(
            src_ref=src, dst_ref=dst, send_sem=ss, recv_sem=rs, device_id=dev, device_id_type=MESH)

    def send(src, dst, ss, rs, dev):
        d = copy(src, dst, ss, rs, dev)
        d.start()
        drain.append((None, d))

    def send_if(cond, src, dst, ss, rs, dev):
        d = copy(src, dst, ss, rs, dev)
        pl.when(cond)(d.start)
        drain.append((cond, d))

    def arrived(region, ss, rs):
        copy(region, region, ss, rs, sibling).wait_recv()

    loads = [pltpu.make_async_copy(s, d, in_sem.at[i])
             for i, (s, d) in enumerate(((gain, gv), (gw, gs), (uw, us), (dw, ds), (tok, X)))]
    for l in loads:
        l.start()
    barrier = pltpu.get_barrier_semaphore()
    greet = [*near[0], *near[1], sibling, {"tp": ring(x, 1)}, {"tp": ring(x, 2)}, {"tp": ring(x, 3)}]
    for dev in greet:
        pl.semaphore_signal(barrier, inc=1, device_id=dev, device_id_type=MESH)

    for l in loads[:3]:
        l.wait()
    eye = lax.broadcasted_iota(jnp.int32, (rows, rows), 0) == lax.broadcasted_iota(jnp.int32, (rows, rows), 1)
    column = jnp.sum(jnp.where(eye, gv[...], 0.0), axis=1, keepdims=True)
    W[0, z, y, c] = (gs[...] * column).astype(bf16)
    W[1, z, y, c] = (us[...] * column).astype(bf16)
    pl.semaphore_wait(barrier, len(greet))

    def region(a, first, second, part=None, k=None):
        zz, yy = (ring(z, first), ring(y, second)) if a == 0 else (ring(z, second), ring(y, first))
        cols = slice(None) if k is None else pl.ds(*CHUNKS[k])
        lead = slice(None) if part is None else part
        return W.at[lead, zz, yy, c, pl.ds(a * half, half), cols]

    def row_of(a, second, core, k):
        cols = pl.ds(*CHUNKS[k])
        if a == 0:
            return W.at[:, :, ring(y, second), core, pl.ds(0, half), cols]
        return W.at[:, ring(z, second), :, core, pl.ds(half, half), cols]

    def p1_send():
        for d in (0, 1):
            for a in (0, 1):
                r = region(a, 0, 0)
                send(r, r, p1s.at[a, d], p1r.at[a, d], near[a][d])

    def p1_forward():
        for d in (0, 1):
            for a in (0, 1):
                arrived(region(a, 3 - 2 * d, 0), p1s.at[a, d], p1r.at[a, d])
                r = region(a, 3 - 2 * d, 0, d)
                send(r, r, p1s.at[a, 2 + d], p1r.at[a, 2 + d], near[a][d])

    def p1_finish():
        for d in (0, 1):
            for a in (0, 1):
                arrived(region(a, 2, 0, d), p1s.at[a, 2 + d], p1r.at[a, 2 + d])

    def p2_send(k, js):
        for j in js:
            for d in (0, 1):
                for a in (0, 1):
                    r = region(a, j, 0, None, k)
                    send(r, r, p2s.at[k, a, d, j], p2r.at[k, a, d, j], near[1 - a][d])

    def p2_forward(k):
        for j in (0, 1, 3, 2):
            for d in (0, 1):
                for a in (0, 1):
                    arrived(region(a, j, 3 - 2 * d, None, k), p2s.at[k, a, d, j], p2r.at[k, a, d, j])
                    r = region(a, j, 3 - 2 * d, d, k)
                    send(r, r, p2s.at[k, a, 2 + d, j], p2r.at[k, a, 2 + d, j], near[1 - a][d])

    def p2_finish(k):
        for j in (0, 1, 3, 2):
            for d in (0, 1):
                for a in (0, 1):
                    arrived(region(a, j, 2, d, k), p2s.at[k, a, 2 + d, j], p2r.at[k, a, 2 + d, j])

    def sib_send(k, seconds):
        for s in seconds:
            for a in (0, 1):
                r = row_of(a, s, c, k)
                send(r, r, sbs.at[k, a, s], sbr.at[k, a, s], sibling)

    def sib_finish(k):
        for s in range(RING):
            for a in (0, 1):
                arrived(row_of(a, s, 1 - c, k), sbs.at[k, a, s], sbr.at[k, a, s])

    def hidden(k):
        start, width = CHUNKS[k]

        def body(t, _):
            at_rows = pl.ds(pl.multiple_of(t * TILE, TILE), TILE)
            a = X[at_rows, :]
            wg = W[0, :, :, :, :, pl.ds(start, width)].reshape(-1, width)
            wu = W[1, :, :, :, :, pl.ds(start, width)].reshape(-1, width)
            g = jnp.dot(a, wg, preferred_element_type=f32)
            u = jnp.dot(a, wu, preferred_element_type=f32)
            H[at_rows, pl.ds(start, width)] = (g / (1.0 + jnp.exp(-g)) * u).astype(bf16)
            return 0

        lax.fori_loop(0, X.shape[0] // TILE, body, 0)

    def place(q):
        return pl.multiple_of(q * dcols, dcols)

    def piece_cols(i):
        off, p = OFFS[i]
        return pl.ds(pl.multiple_of(ring(x, off) * dcols + p * PIECE, PIECE), PIECE)

    def d0_send():
        loads[3].wait()
        mine = pl.ds(place(x), dcols)
        own = ds[...].astype(bf16)
        dst[...] = own

        @pl.when(x == z)
        def _():
            Dn[y, c, :, mine] = own

        send_if(x != z, dst, Dn.at[y, c, :, mine], d0s.at[0], d0r.at[x], {"tp": z})

    def d0_finish():
        for k in (1, 2, 3):
            q = ring(x, k)
            pl.when(x == z)(lambda q=q: arrived(Dn.at[y, c, :, pl.ds(place(q), dcols)], d0s.at[0], d0r.at[q]))

    lo, hi = pl.ds(0, dcut), pl.ds(dcut, drows - dcut)
    cuts = (lo, hi)

    def d1_send(i):
        r = Dn.at[y, c, :, piece_cols(i)]
        for d in (0, 1):
            send_if(z == x, r, r, d1s.at[i, d], d1r.at[i, d], near[0][d])

    def d1_forward(i):
        cols = piece_cols(i)
        for d in (0, 1):
            here = z == ring(x, 1 + 2 * d)
            pl.when(here)(lambda d=d: arrived(Dn.at[y, c, :, cols], d1s.at[i, d], d1r.at[i, d]))
            r = Dn.at[y, c, cuts[d], cols]
            send_if(here, r, r, d1s.at[i, 2 + d], d1r.at[i, 2 + d], near[0][d])
        for d in (0, 1):
            pl.when(z == ring(x, 2))(
                lambda d=d: arrived(Dn.at[y, c, cuts[d], cols], d1s.at[i, 2 + d], d1r.at[i, 2 + d]))

    def d2_send(i):
        r = Dn.at[y, c, :, piece_cols(i)]
        for d in (0, 1):
            send(r, r, d2s.at[i, d], d2r.at[i, d], near[1][d])

    def d2_forward(i):
        cols = piece_cols(i)
        for d in (0, 1):
            yy = ring(y, 3 - 2 * d)
            arrived(Dn.at[yy, c, :, cols], d2s.at[i, d], d2r.at[i, d])
            r = Dn.at[yy, c, cuts[d], cols]
            send(r, r, d2s.at[i, 2 + d], d2r.at[i, 2 + d], near[1][d])

    def d2_finish(i):
        cols = piece_cols(i)
        for d in (0, 1):
            arrived(Dn.at[ring(y, 2), c, cuts[d], cols], d2s.at[i, 2 + d], d2r.at[i, 2 + d])
        r = Dn.at[:, c, :, cols]
        send(r, r, dbs.at[i], dbr.at[i], sibling)

    def d_ready(i):
        arrived(Dn.at[:, 1 - c, :, piece_cols(i)], dbs.at[i], dbr.at[i])

    def share(i):
        off, p = OFFS[i]
        cols = piece_cols(i)
        hw = PIECE // 2
        if off == 1:
            arrived(R2.at[p, 0], rss.at[0, p, 0], rsr.at[0, p, 0])
        if off == 3:
            arrived(R2.at[p, 1], rss.at[0, p, 1], rsr.at[0, p, 1])
        if off == 0:
            for d in (0, 1):
                arrived(R1.at[p, d], rss.at[1, p, d], rsr.at[1, p, d])

        def body(t, _):
            at_rows = pl.ds(pl.multiple_of(t * TILE, TILE), TILE)
            w = Dn[:, :, :, cols].reshape(-1, PIECE)
            v = jnp.dot(H[at_rows, :], w, preferred_element_type=f32)
            if off == 2:
                v = v.astype(bf16)
                S2[p, 0, at_rows, :] = v[:, hw:]
                S2[p, 1, at_rows, :] = v[:, :hw]
            elif off == 1:
                S1[p, 0, at_rows, pl.ds(0, hw)] = v[:, :hw].astype(bf16)
                S1[p, 0, at_rows, pl.ds(hw, hw)] = (v[:, hw:] + R2[p, 0, at_rows, :].astype(f32)).astype(bf16)
            elif off == 3:
                S1[p, 1, at_rows, pl.ds(0, hw)] = (v[:, :hw] + R2[p, 1, at_rows, :].astype(f32)).astype(bf16)
                S1[p, 1, at_rows, pl.ds(hw, hw)] = v[:, hw:].astype(bf16)
            else:
                v = v + R1[p, 0, at_rows, :].astype(f32) + R1[p, 1, at_rows, :].astype(f32)
                mixed[at_rows, pl.ds(p * PIECE, PIECE)] = v.astype(bf16)
            return 0

        lax.fori_loop(0, H.shape[0] // TILE, body, 0)
        if off == 2:
            for d in (0, 1):
                send(S2.at[p, d], R2.at[p, d], rss.at[0, p, d], rsr.at[0, p, d], xnear[d])
        if off in (1, 3):
            d = (off - 1) // 2
            send(S1.at[p, d], R1.at[p, d], rss.at[1, p, d], rsr.at[1, p, d], xnear[d])

    def norm():
        loads[4].wait()
        step = 32

        def body(t, _):
            at_rows = pl.ds(pl.multiple_of(t * step, step), step)
            v = X[at_rows, :].astype(f32)
            m = jnp.mean(v * v, axis=-1, keepdims=True)
            X[at_rows, :] = (v * lax.rsqrt(m + eps_norm)).astype(bf16)
            return 0

        lax.fori_loop(0, X.shape[0] // step, body, 0)

    p1_send()
    p2_send(0, (0,))
    p2_send(1, (0,))
    d0_send()
    norm()
    p1_forward()
    p2_send(0, (1, 3))
    p2_send(1, (1, 3))
    p1_finish()
    p2_send(0, (2,))
    p2_send(1, (2,))
    p2_send(2, (0,))
    d0_finish()
    for k in range(NCH):
        p2_forward(k)
        sib_send(k, (0, 1, 3))
        if k + 2 < NCH:
            p2_send(k + 2, (1, 3, 2))
        if k + 3 < NCH:
            p2_send(k + 3, (0,))
        if k == NCH - 2:
            d1_send(0)
            d1_send(1)
        if k == NCH - 1:
            d1_forward(0)
            d2_send(0)
            for i in range(2, NP):
                d1_send(i)
        if k:
            sib_finish(k - 1)
            hidden(k - 1)
        p2_finish(k)
        sib_send(k, (2,))
    d1_forward(1)
    d2_send(1)
    d2_forward(0)
    sib_finish(NCH - 1)
    hidden(NCH - 1)
    d2_finish(0)
    for i in range(NP):
        if i + 2 < NP:
            d1_forward(i + 2)
            d2_send(i + 2)
        if i + 1 < NP:
            d2_forward(i + 1)
            d2_finish(i + 1)
        d_ready(i)
        share(i)
    for cond, d in drain:
        if cond is None:
            d.wait_send()
        else:
            pl.when(cond)(d.wait_send)


def write_out(W, Dn, m, g_out, u_out, d_out, m_out, sem):
    copies = [pltpu.make_async_copy(s, d, sem.at[i])
              for i, (s, d) in enumerate(((W.at[0], g_out), (W.at[1], u_out), (Dn, d_out), (m, m_out)))]
    for c in copies:
        c.start()
    for c in copies:
        c.wait()


def on_device(tokens, norm_gain, gate_weight, up_weight, down_weight):
    toks, width = tokens.shape
    rows, ff = gate_weight.shape
    drows, dcols = down_weight.shape
    hbm = pl.BlockSpec(memory_space=pltpu.HBM)
    vmem = pl.BlockSpec(memory_space=pltpu.VMEM)
    dma = pltpu.SemaphoreType.DMA
    half_piece = PIECE // 2
    W, Dn, m = pl.pallas_call(
        kernel,
        out_shape=(
            pltpu.VMEM((2, RING, RING, 2, rows, ff), bf16),
            pltpu.VMEM((RING, 2, drows, width), bf16),
            pltpu.VMEM((toks, dcols), bf16),
        ),
        in_specs=[hbm] * 5,
        out_specs=(vmem,) * 3,
        scratch_shapes=[
            pltpu.VMEM((toks, width), bf16),
            pltpu.VMEM((toks, ff), bf16),
            pltpu.VMEM((rows, ff), f32),
            pltpu.VMEM((rows, ff), f32),
            pltpu.VMEM((drows, dcols), f32),
            pltpu.VMEM((drows, dcols), bf16),
            pltpu.VMEM((1, rows), f32),
            pltpu.VMEM((2, 2, toks, half_piece), bf16),
            pltpu.VMEM((2, 2, toks, PIECE), bf16),
            pltpu.VMEM((2, 2, toks, half_piece), bf16),
            pltpu.VMEM((2, 2, toks, PIECE), bf16),
            dma((5,)),
            dma((2, 4)), dma((2, 4)),
            dma((NCH, 2, 4, RING)), dma((NCH, 2, 4, RING)),
            dma((NCH, 2, RING)), dma((NCH, 2, RING)),
            dma((1,)), dma((RING,)),
            dma((NP, 4)), dma((NP, 4)),
            dma((NP, 4)), dma((NP, 4)),
            dma((NP,)), dma((NP,)),
            dma((2, 2, 2)), dma((2, 2, 2)),
        ],
        compiler_params=pltpu.CompilerParams(
            collective_id=0, has_side_effects=True, vmem_limit_bytes=36 * 2**20),
    )(tokens, norm_gain.reshape(1, rows), gate_weight, up_weight, down_weight)
    return pl.pallas_call(
        write_out,
        out_shape=(
            jax.ShapeDtypeStruct((width, ff), bf16),
            jax.ShapeDtypeStruct((width, ff), bf16),
            jax.ShapeDtypeStruct((ff, width), bf16),
            jax.ShapeDtypeStruct((toks, dcols), bf16),
        ),
        in_specs=[vmem] * 3,
        out_specs=(hbm,) * 4,
        scratch_shapes=[dma((4,))],
        compiler_params=pltpu.CompilerParams(vmem_limit_bytes=2**20),
    )(W.reshape(2, width, ff), Dn.reshape(ff, width), m)


def solution(mesh):
    in_specs = (P("fs", None), P("fs"), P("fs", "tp"), P("fs", "tp"), P("fs", "tp"))
    out_specs = (P(None, "tp"), P(None, "tp"), P("tp", None), P("fs", "tp"))
    return jax.shard_map(
        on_device, mesh=mesh, in_specs=in_specs, out_specs=out_specs, check_vma=False
    )
```

```python
import jax
import jax.numpy as jnp
from jax import lax
from jax.experimental import pallas as pl
from jax.experimental.pallas import tpu as pltpu
from jax.sharding import PartitionSpec as P

MESH = pl.DeviceIdType.MESH
bf16, f32 = jnp.bfloat16, jnp.float32
eps_norm = 1e-06
RING = 4
CHUNKS = ((0, 384), (384, 384), (768, 384), (1152, 256))
NCH = len(CHUNKS)
PARTS = 3
PIECE = 256
OFFS = ((2, 0), (2, 1), (1, 0), (3, 0), (1, 1), (3, 1), (0, 0), (0, 1))
NP = len(OFFS)
TILE = 256
ORDER = (
    "P1S", "P2S.1.0", "P2S.0.0", "P1F", "D0S", "NORM.0", "P2S.2.0", "P2S.0.3", "P2S.1.1", "P2S.0.1",
    "P2S.2.1", "P1E", "P2S.1.2", "P2S.1.3", "P2S.2.2", "P2S.3.0", "P2S.0.2", "NORM.1", "P2S.2.3", "D0",
    "D1S.0", "P2F.1", "P2F.0", "D1F.0", "P2F.2", "P2E.1", "P2S.3.1", "P2S.3.3", "P2S.3.2", "D1E.0", "D1S.1",
    "NORM.2", "P2E.0", "HID.1.0", "D1S.2", "D2S.0", "P2E.2", "HID.0.0", "HID.0.1", "P2F.3", "D1S.3",
    "HID.1.1", "D2F.0", "D1S.4", "D1F.1", "HID.2.0", "HID.0.2", "D1F.2", "D2E.0", "D1S.5", "HID.2.1",
    "D1E.1", "D2S.1", "D1S.6", "P2E.3", "HID.1.2", "D1E.2", "D1F.3", "HID.3.0", "D2S.2", "D1S.7", "HID.2.2",
    "D1F.4", "HID.3.1", "D2F.1", "D1E.3", "HID.3.2", "D2S.3", "SH.0", "D1E.4", "D2F.2", "D1F.5", "D2E.1",
    "D2S.4", "D1F.6", "D2F.3", "SH.1", "D2E.2", "D1E.5", "D1E.6", "D2F.4", "D2S.5", "D1F.7", "D2S.6",
    "D2E.3", "SH.2", "SH.3", "D2E.4", "D2F.5", "D1E.7", "SH.4", "D2S.7", "D2F.6", "D2E.5", "SH.5", "D2F.7",
    "D2E.7", "D2E.6", "SH.6", "SH.7",
)


def ring(v, k):
    return lax.rem(v + k, RING)


def kernel(tok, gain, gw, uw, dw, W, Dn, mixed, X, H, gs, us, ds, dst, gv, S2, S1, R2, R1,
           in_sem, p1s, p1r, p2s, p2r, sbs, sbr, d0s, d0r, d1s, d1r, d2s, d2r, dbs, dbr, rss, rsr):
    x = lax.axis_index("tp")
    f = lax.axis_index("fs")
    c = lax.rem(f, 2)
    y = lax.rem(lax.div(f, 2), RING)
    z = lax.div(f, 2 * RING)
    rows, half = gs.shape[0], gs.shape[0] // 2
    drows, dcols = ds.shape
    dcut = 96

    def at(zz, yy, cc):
        return {"fs": (zz * RING + yy) * 2 + cc}

    zp, zm, yp, ym = ring(z, 1), ring(z, 3), ring(y, 1), ring(y, 3)
    near = ((at(zp, y, c), at(zm, y, c)), (at(z, yp, c), at(z, ym, c)))
    sibling = at(z, y, 1 - c)
    xnear = ({"tp": ring(x, 1)}, {"tp": ring(x, 3)})

    drain = []

    def copy(src, dst, ss, rs, dev):
        return pltpu.make_async_remote_copy(
            src_ref=src, dst_ref=dst, send_sem=ss, recv_sem=rs, device_id=dev, device_id_type=MESH)

    def send(src, dst, ss, rs, dev):
        d = copy(src, dst, ss, rs, dev)
        d.start()
        drain.append((None, d))

    def send_if(cond, src, dst, ss, rs, dev):
        d = copy(src, dst, ss, rs, dev)
        pl.when(cond)(d.start)
        drain.append((cond, d))

    def arrived(region, ss, rs):
        copy(region, region, ss, rs, sibling).wait_recv()

    loads = [pltpu.make_async_copy(s, d, in_sem.at[i])
             for i, (s, d) in enumerate(((gain, gv), (gw, gs), (uw, us), (dw, ds), (tok, X)))]
    for l in loads:
        l.start()
    barrier = pltpu.get_barrier_semaphore()
    greet = [*near[0], *near[1], sibling, {"tp": ring(x, 1)}, {"tp": ring(x, 2)}, {"tp": ring(x, 3)}]
    for dev in greet:
        pl.semaphore_signal(barrier, inc=1, device_id=dev, device_id_type=MESH)

    for l in loads[:3]:
        l.wait()
    eye = lax.broadcasted_iota(jnp.int32, (rows, rows), 0) == lax.broadcasted_iota(jnp.int32, (rows, rows), 1)
    column = jnp.sum(jnp.where(eye, gv[...], 0.0), axis=1, keepdims=True)
    W[0, z, y, c] = (gs[...] * column).astype(bf16)
    W[1, z, y, c] = (us[...] * column).astype(bf16)
    pl.semaphore_wait(barrier, len(greet))

    def cols_of(k):
        return slice(None) if k is None else pl.ds(*CHUNKS[k])

    def region(a, first, second, part=None, k=None):
        zz, yy = (ring(z, first), ring(y, second)) if a == 0 else (ring(z, second), ring(y, first))
        lead = slice(None) if part is None else part
        return W.at[lead, zz, yy, c, pl.ds(a * half, half), cols_of(k)]

    def line(a, second, core, k, part=None):
        lead = slice(None) if part is None else part
        if a == 0:
            return W.at[lead, :, ring(y, second), core, pl.ds(0, half), cols_of(k)]
        return W.at[lead, ring(z, second), :, core, pl.ds(half, half), cols_of(k)]

    def begin(src, ss, rs, dev):
        copy(src, src, ss, rs, dev).start()

    def sent(region_sent, ss):
        drain.append((None, copy(region_sent, region_sent, ss, ss, sibling)))

    def P1S():
        for d in (0, 1):
            for a in (0, 1):
                begin(region(a, 0, 0), p1s.at[a, d], p1r.at[a, d], near[a][d])
                sent(region(a, 0, 0), p1s.at[a, d])

    def P1F():
        for d in (0, 1):
            for a in (0, 1):
                arrived(region(a, 3 - 2 * d, 0), p1s.at[a, d], p1r.at[a, d])
                r = region(a, 3 - 2 * d, 0, d)
                begin(r, p1s.at[a, 2 + d], p1r.at[a, 2 + d], near[a][d])
                sent(r, p1s.at[a, 2 + d])

    def P1E():
        for d in (0, 1):
            for a in (0, 1):
                arrived(region(a, 2, 0, d), p1s.at[a, 2 + d], p1r.at[a, 2 + d])

    def P2S(k, j):
        for d in (0, 1):
            for a in (0, 1):
                begin(region(a, j, 0, None, k), p2s.at[k, a, d], p2r.at[k, a, d], near[1 - a][d])
                if j == 0:
                    sent(line(a, 0, c, k), p2s.at[k, a, d])

    def sib(k, second):
        for a in (0, 1):
            begin(line(a, second, c, k), sbs.at[k], sbr.at[k], sibling)

    def P2F(k):
        for d in (0, 1):
            for a in (0, 1):
                arrived(line(a, 3 - 2 * d, c, k), p2s.at[k, a, d], p2r.at[k, a, d])
                r = line(a, 3 - 2 * d, c, k, d)
                begin(r, p2s.at[k, a, 2 + d], p2r.at[k, a, 2 + d], near[1 - a][d])
                sent(r, p2s.at[k, a, 2 + d])
        for second in (0, 1, 3):
            sib(k, second)

    def P2E(k):
        for d in (0, 1):
            for a in (0, 1):
                arrived(line(a, 2, c, k, d), p2s.at[k, a, 2 + d], p2r.at[k, a, 2 + d])
        sib(k, 2)
        sent(W.at[:, :, :, c, :, cols_of(k)], sbs.at[k])

    def HID(k, t):
        if t == 0:
            arrived(W.at[:, :, :, 1 - c, :, cols_of(k)], sbs.at[k], sbr.at[k])
        start, width = CHUNKS[k]
        tile = X.shape[0] // PARTS
        at_rows = pl.ds(t * tile, tile)
        cols = pl.ds(start, width)
        w = jnp.concatenate([W[0, :, :, :, :, cols].reshape(-1, width), W[1, :, :, :, :, cols].reshape(-1, width)], axis=1)
        v = jnp.dot(X[at_rows, :], w, preferred_element_type=f32)
        g, u = v[:, :width], v[:, width:]
        H[at_rows, cols] = (g / (1.0 + jnp.exp(-g)) * u).astype(bf16)

    def place(q):
        return pl.multiple_of(q * dcols, dcols)

    def piece_cols(i):
        off, p = OFFS[i]
        return pl.ds(pl.multiple_of(ring(x, off) * dcols + p * PIECE, PIECE), PIECE)

    def D0S():
        loads[3].wait()
        mine = pl.ds(place(x), dcols)
        own = ds[...].astype(bf16)
        dst[...] = own

        @pl.when(x == z)
        def _():
            Dn[y, c, :, mine] = own

        send_if(x != z, dst, Dn.at[y, c, :, mine], d0s.at[0], d0r.at[x], {"tp": z})

    def D0():
        for k in (1, 2, 3):
            q = ring(x, k)
            pl.when(x == z)(lambda q=q: arrived(Dn.at[y, c, :, pl.ds(place(q), dcols)], d0s.at[0], d0r.at[q]))

    lo, hi = pl.ds(0, dcut), pl.ds(dcut, drows - dcut)
    cuts = (lo, hi)

    def all_sent(i, cond, r, ss):
        if i == NP - 1:
            drain.append((cond, copy(r, r, ss, ss, sibling)))

    def D1S(i):
        for d in (0, 1):
            r = Dn.at[y, c, :, piece_cols(i)]
            pl.when(z == x)(copy(r, r, d1s.at[d], d1r.at[i, d], near[0][d]).start)
            all_sent(i, z == x, Dn.at[y, c, :, :], d1s.at[d])

    def D1F(i):
        for d in (0, 1):
            here = z == ring(x, 1 + 2 * d)

            @pl.when(here)
            def _():
                arrived(Dn.at[y, c, :, piece_cols(i)], d1s.at[d], d1r.at[i, d])
                begin(Dn.at[y, c, cuts[d], piece_cols(i)], d1s.at[2 + d], d1r.at[i, 2 + d], near[0][d])

            all_sent(i, here, Dn.at[y, c, cuts[d], :], d1s.at[2 + d])

    def D1E(i):
        @pl.when(z == ring(x, 2))
        def _():
            for d in (0, 1):
                arrived(Dn.at[y, c, cuts[d], piece_cols(i)], d1s.at[2 + d], d1r.at[i, 2 + d])

    def D2S(i):
        for d in (0, 1):
            begin(Dn.at[y, c, :, piece_cols(i)], d2s.at[d], d2r.at[i, d], near[1][d])
            all_sent(i, None, Dn.at[y, c, :, :], d2s.at[d])

    def D2F(i):
        for d in (0, 1):
            yy = ring(y, 3 - 2 * d)
            arrived(Dn.at[yy, c, :, piece_cols(i)], d2s.at[d], d2r.at[i, d])
            begin(Dn.at[yy, c, cuts[d], piece_cols(i)], d2s.at[2 + d], d2r.at[i, 2 + d], near[1][d])
            all_sent(i, None, Dn.at[yy, c, cuts[d], :], d2s.at[2 + d])

    def D2E(i):
        for d in (0, 1):
            arrived(Dn.at[ring(y, 2), c, cuts[d], piece_cols(i)], d2s.at[2 + d], d2r.at[i, 2 + d])
        begin(Dn.at[:, c, :, piece_cols(i)], dbs.at[0], dbr.at[i], sibling)
        all_sent(i, None, Dn.at[:, c, :, :], dbs.at[0])

    def SH(i):
        arrived(Dn.at[:, 1 - c, :, piece_cols(i)], dbs.at[0], dbr.at[i])
        off, p = OFFS[i]
        cols = piece_cols(i)
        hw = PIECE // 2
        if off == 1:
            arrived(R2.at[p, 0], rss.at[0, p, 0], rsr.at[0, p, 0])
        if off == 3:
            arrived(R2.at[p, 1], rss.at[0, p, 1], rsr.at[0, p, 1])
        if off == 0:
            for d in (0, 1):
                arrived(R1.at[p, d], rss.at[1, p, d], rsr.at[1, p, d])

        def body(t, _):
            at_rows = pl.ds(pl.multiple_of(t * TILE, TILE), TILE)
            w = Dn[:, :, :, cols].reshape(-1, PIECE)
            v = jnp.dot(H[at_rows, :], w, preferred_element_type=f32)
            if off == 2:
                v = v.astype(bf16)
                S2[p, 0, at_rows, :] = v[:, hw:]
                S2[p, 1, at_rows, :] = v[:, :hw]
            elif off == 1:
                S1[p, 0, at_rows, pl.ds(0, hw)] = v[:, :hw].astype(bf16)
                S1[p, 0, at_rows, pl.ds(hw, hw)] = (v[:, hw:] + R2[p, 0, at_rows, :].astype(f32)).astype(bf16)
            elif off == 3:
                S1[p, 1, at_rows, pl.ds(0, hw)] = (v[:, :hw] + R2[p, 1, at_rows, :].astype(f32)).astype(bf16)
                S1[p, 1, at_rows, pl.ds(hw, hw)] = v[:, hw:].astype(bf16)
            else:
                v = v + R1[p, 0, at_rows, :].astype(f32) + R1[p, 1, at_rows, :].astype(f32)
                mixed[at_rows, pl.ds(p * PIECE, PIECE)] = v.astype(bf16)
            return 0

        lax.fori_loop(0, H.shape[0] // TILE, body, 0)
        if off == 2:
            for d in (0, 1):
                send(S2.at[p, d], R2.at[p, d], rss.at[0, p, d], rsr.at[0, p, d], xnear[d])
        if off in (1, 3):
            d = (off - 1) // 2
            send(S1.at[p, d], R1.at[p, d], rss.at[1, p, d], rsr.at[1, p, d], xnear[d])

    def NORM(t):
        if t == 0:
            loads[4].wait()
        step = 32
        count = X.shape[0] // 3 // step

        def body(i, _):
            at_rows = pl.ds(pl.multiple_of((t * count + i) * step, step), step)
            v = X[at_rows, :].astype(f32)
            m = jnp.mean(v * v, axis=-1, keepdims=True)
            X[at_rows, :] = (v * lax.rsqrt(m + eps_norm)).astype(bf16)
            return 0

        lax.fori_loop(0, count, body, 0)

    does = {f.__name__: f for f in (P1S, P1F, P1E, P2S, P2F, P2E, HID, NORM, D0S, D0, D1S, D1F, D1E, D2S, D2F, D2E, SH)}
    for word in ORDER:
        name, *numbers = word.split(".")
        does[name](*map(int, numbers))
    for cond, d in drain:
        if cond is None:
            d.wait_send()
        else:
            pl.when(cond)(d.wait_send)


def write_out(W, Dn, m, g_out, u_out, d_out, m_out, sem):
    copies = [pltpu.make_async_copy(s, d, sem.at[i])
              for i, (s, d) in enumerate(((W.at[0], g_out), (W.at[1], u_out), (Dn, d_out), (m, m_out)))]
    for c in copies:
        c.start()
    for c in copies:
        c.wait()


def on_device(tokens, norm_gain, gate_weight, up_weight, down_weight):
    toks, width = tokens.shape
    rows, ff = gate_weight.shape
    drows, dcols = down_weight.shape
    hbm = pl.BlockSpec(memory_space=pltpu.HBM)
    vmem = pl.BlockSpec(memory_space=pltpu.VMEM)
    dma = pltpu.SemaphoreType.DMA
    half_piece = PIECE // 2
    W, Dn, m = pl.pallas_call(
        kernel,
        out_shape=(
            pltpu.VMEM((2, RING, RING, 2, rows, ff), bf16),
            pltpu.VMEM((RING, 2, drows, width), bf16),
            pltpu.VMEM((toks, dcols), bf16),
        ),
        in_specs=[hbm] * 5,
        out_specs=(vmem,) * 3,
        scratch_shapes=[
            pltpu.VMEM((toks, width), bf16),
            pltpu.VMEM((toks, ff), bf16),
            pltpu.VMEM((rows, ff), f32),
            pltpu.VMEM((rows, ff), f32),
            pltpu.VMEM((drows, dcols), f32),
            pltpu.VMEM((drows, dcols), bf16),
            pltpu.VMEM((1, rows), f32),
            pltpu.VMEM((2, 2, toks, half_piece), bf16),
            pltpu.VMEM((2, 2, toks, PIECE), bf16),
            pltpu.VMEM((2, 2, toks, half_piece), bf16),
            pltpu.VMEM((2, 2, toks, PIECE), bf16),
            dma((5,)),
            dma((2, 4)), dma((2, 4)),
            dma((NCH, 2, 4)), dma((NCH, 2, 4)),
            dma((NCH,)), dma((NCH,)),
            dma((1,)), dma((RING,)),
            dma((4,)), dma((NP, 4)),
            dma((4,)), dma((NP, 4)),
            dma((1,)), dma((NP,)),
            dma((2, 2, 2)), dma((2, 2, 2)),
        ],
        compiler_params=pltpu.CompilerParams(
            collective_id=0, has_side_effects=True, vmem_limit_bytes=48_900_000),
    )(tokens, norm_gain.reshape(1, rows), gate_weight, up_weight, down_weight)
    return pl.pallas_call(
        write_out,
        out_shape=(
            jax.ShapeDtypeStruct((width, ff), bf16),
            jax.ShapeDtypeStruct((width, ff), bf16),
            jax.ShapeDtypeStruct((ff, width), bf16),
            jax.ShapeDtypeStruct((toks, dcols), bf16),
        ),
        in_specs=[vmem] * 3,
        out_specs=(hbm,) * 4,
        scratch_shapes=[dma((4,))],
        compiler_params=pltpu.CompilerParams(vmem_limit_bytes=2**20),
    )(W.reshape(2, width, ff), Dn.reshape(ff, width), m)


def solution(mesh):
    in_specs = (P("fs", None), P("fs"), P("fs", "tp"), P("fs", "tp"), P("fs", "tp"))
    out_specs = (P(None, "tp"), P(None, "tp"), P("tp", None), P("fs", "tp"))
    return jax.shard_map(
        on_device, mesh=mesh, in_specs=in_specs, out_specs=out_specs, check_vma=False
    )
```

```python
import jax
import jax.numpy as jnp
from jax import lax
from jax.experimental import pallas as pl
from jax.experimental.pallas import tpu as pltpu
from jax.sharding import PartitionSpec as P

MESH = pl.DeviceIdType.MESH
bf16, f32 = jnp.bfloat16, jnp.float32
eps_norm = 1e-06
RING = 4
CHUNKS = ((0, 384), (384, 256), (640, 256), (896, 256), (1152, 256))
NCH = len(CHUNKS)
PARTS = 2
PIECE = 256
OFFS = ((2, 0), (2, 1), (1, 0), (3, 0), (1, 1), (3, 1), (0, 0), (0, 1))
NP = len(OFFS)
TILE = 256
ORDER = (
    "P1S.0", "P1S.1", "P1S.2", "P2S.0.0", "P1S.3", "P2S.4.0", "P2S.3.0", "D0S.0", "NORM.0", "P1S.4",
    "P1F.0", "P1F.2", "P2S.2.3", "P2S.0.3", "P1F.4", "P2S.2.0", "P1E.0", "P1E.2", "D0S.1", "P1F.3",
    "P2S.0.1", "P2S.4.1", "NORM.1", "P2S.2.1", "P2S.0.2", "D0.0", "P1F.1", "NORM.2", "P2S.1.3", "D1S.0",
    "P1E.4", "P2S.4.2", "P2S.4.3", "P1E.1", "P2S.2.2", "P2F.0", "P2S.1.1", "D0.1", "D1F.0", "P2S.1.2",
    "D1S.1", "P2S.3.3", "P2E.0", "P2S.1.0", "P2F.4", "P2S.3.1", "P1E.3", "P2S.3.2", "D1E.0", "D1F.1",
    "D2S.0", "P2F.2", "HID.0.0", "P2E.4", "D1E.1", "D1S.2", "D2S.1", "P2F.3", "HID.0.1", "P2E.2", "D1S.3",
    "D2F.0", "P2F.1", "HID.4.0", "D1S.4", "D1F.2", "HID.4.1", "HID.2.0", "D2F.1", "P2E.3", "D1S.5",
    "HID.2.1", "D1F.3", "D1E.2", "D2S.2", "D2E.0", "HID.3.0", "P2E.1", "HID.3.1", "D1S.6", "D1S.7", "D1E.3",
    "D2S.3", "D2E.1", "HID.1.0", "HID.1.1", "D1F.4", "SH.0", "D1F.5", "D2F.2", "SH.1", "D2F.3", "D1E.4",
    "D2S.4", "D1F.6", "D1F.7", "D2E.2", "D1E.5", "D2S.5", "D2E.3", "D1E.6", "D2S.6", "SH.2", "SH.3",
    "D2F.4", "D1E.7", "D2S.7", "D2F.5", "D2F.6", "D2E.4", "D2F.7", "SH.4", "D2E.5", "D2E.6", "D2E.7",
    "SH.5", "SH.6", "SH.7",
)


def ring(v, k):
    return lax.rem(v + k, RING)


def kernel(tok, gain, gw, uw, dw, W, Dn, H, R1, Tp, Tm, X, gs, us, ds, dst, gv, S2, S1, R2,
           in_sem, out_sem, sib_sem, gu_sem, d0_sem, d_sem, r2_sem, r1_sem):
    x = lax.axis_index("tp")
    f = lax.axis_index("fs")
    c = lax.rem(f, 2)
    y = lax.rem(lax.div(f, 2), RING)
    z = lax.div(f, 2 * RING)
    rows, half = gs.shape[0], gs.shape[0] // 2
    drows, dcols = ds.shape
    dcut = 96

    def at(zz, yy, cc):
        return {"fs": (zz * RING + yy) * 2 + cc}

    zp, zm, yp, ym = ring(z, 1), ring(z, 3), ring(y, 1), ring(y, 3)
    near = ((at(zp, y, c), at(zm, y, c)), (at(z, yp, c), at(z, ym, c)))
    sibling = at(z, y, 1 - c)
    xnear = ({"tp": ring(x, 1)}, {"tp": ring(x, 3)})

    drain = []

    def copy(src, dst, ss, rs, dev):
        return pltpu.make_async_remote_copy(
            src_ref=src, dst_ref=dst, send_sem=ss, recv_sem=rs, device_id=dev, device_id_type=MESH)

    def begin(src, ss, rs, dev):
        copy(src, src, ss, rs, dev).start()

    def arrived(view, rs):
        copy(view, view, out_sem.at[0], rs, sibling).wait_recv()

    def sent(view, ss, cond=None):
        drain.append((cond, copy(view, view, ss, ss, sibling)))

    loads = [pltpu.make_async_copy(s, d, in_sem.at[i])
             for i, (s, d) in enumerate(((gain, gv), (gw, gs), (uw, us), (dw, ds), (tok, X)))]
    for l in loads:
        l.start()
    barrier = pltpu.get_barrier_semaphore()
    greet = [*near[0], *near[1], sibling, {"tp": ring(x, 1)}, {"tp": ring(x, 2)}, {"tp": ring(x, 3)}]
    for dev in greet:
        pl.semaphore_signal(barrier, inc=1, device_id=dev, device_id_type=MESH)

    for l in loads[:3]:
        l.wait()
    eye = lax.broadcasted_iota(jnp.int32, (rows, rows), 0) == lax.broadcasted_iota(jnp.int32, (rows, rows), 1)
    column = jnp.sum(jnp.where(eye, gv[...], 0.0), axis=1, keepdims=True)
    W[0, z, y, c] = (gs[...] * column).astype(bf16)
    W[1, z, y, c] = (us[...] * column).astype(bf16)
    pl.semaphore_wait(barrier, len(greet))

    def cols_of(k):
        return pl.ds(*CHUNKS[k])

    def region(a, first, second, part, k):
        zz, yy = (ring(z, first), ring(y, second)) if a == 0 else (ring(z, second), ring(y, first))
        lead = slice(None) if part is None else part
        return W.at[lead, zz, yy, c, pl.ds(a * half, half), cols_of(k)]

    def line(a, second, core, k, part=None):
        lead = slice(None) if part is None else part
        if a == 0:
            return W.at[lead, :, ring(y, second), core, pl.ds(0, half), cols_of(k)]
        return W.at[lead, ring(z, second), :, core, pl.ds(half, half), cols_of(k)]

    def P1S(k):
        for d in (0, 1):
            for a in (0, 1):
                begin(region(a, 0, 0, None, k), out_sem.at[0], gu_sem.at[k, 0], near[a][d])
        if k == 0:
            sent(W.at[:, 0, 0], out_sem.at[0])

    def P1F(k):
        arrived(W.at[:, 0, 0, :, :, cols_of(k)], gu_sem.at[k, 0])
        for d in (0, 1):
            for a in (0, 1):
                begin(region(a, 3 - 2 * d, 0, d, k), out_sem.at[1], gu_sem.at[k, 1], near[a][d])
        if k == 0:
            sent(W.at[0, 0, 0], out_sem.at[1])

    def P1E(k):
        arrived(W.at[0, 0, 0, :, :, cols_of(k)], gu_sem.at[k, 1])

    def P2S(k, j):
        for d in (0, 1):
            for a in (0, 1):
                begin(region(a, j, 0, None, k), out_sem.at[2], gu_sem.at[k, 2], near[1 - a][d])
        if k == 0 and j == 0:
            sent(W.at[:, :, 0], out_sem.at[2])

    def sib(k, second):
        for a in (0, 1):
            begin(line(a, second, c, k), sib_sem.at[0, k], sib_sem.at[1, k], sibling)

    def P2F(k):
        arrived(W.at[:, :, 0, :, :, cols_of(k)], gu_sem.at[k, 2])
        for d in (0, 1):
            for a in (0, 1):
                begin(line(a, 3 - 2 * d, c, k, d), out_sem.at[3], gu_sem.at[k, 3], near[1 - a][d])
        if k == 0:
            sent(W.at[0, :, 0], out_sem.at[3])
        for second in (0, 1, 3):
            sib(k, second)

    def P2E(k):
        arrived(W.at[0, :, 0, :, :, cols_of(k)], gu_sem.at[k, 3])
        sib(k, 2)
        sent(W.at[:, :, :, c, :, cols_of(k)], sib_sem.at[0, k])

    def HID(k, t):
        if t == 0:
            arrived(W.at[:, :, :, 1 - c, :, cols_of(k)], sib_sem.at[1, k])
        start, width = CHUNKS[k]
        tile = X.shape[0] // PARTS
        at_rows = pl.ds(t * tile, tile)
        cols = pl.ds(start, width)
        w = jnp.concatenate([W[0, :, :, :, :, cols].reshape(-1, width), W[1, :, :, :, :, cols].reshape(-1, width)], axis=1)
        v = jnp.dot(X[at_rows, :], w, preferred_element_type=f32)
        g, u = v[:, :width], v[:, width:]
        H[at_rows, cols] = (g / (1.0 + jnp.exp(-g)) * u).astype(bf16)

    def place(q):
        return pl.multiple_of(q * dcols, dcols)

    def piece_cols(i):
        off, p = OFFS[i]
        return pl.ds(pl.multiple_of(ring(x, off) * dcols + p * PIECE, PIECE), PIECE)

    def D0S(late):
        mine = pl.ds(place(x), dcols)
        if not late:
            loads[3].wait()
            rounded = ds[...].astype(bf16)
            dst[...] = rounded

            @pl.when(x == z)
            def _():
                Dn[y, c, :, mine] = rounded

        go = (z == ring(x, 1)) | (z == ring(x, 3)) if late else z == ring(x, 2)
        pl.when(go)(copy(dst, Dn.at[y, c, :, mine], out_sem.at[4], d0_sem.at[late], {"tp": z}).start)
        if late:
            sent(dst, out_sem.at[4], z != x)

    def D0(late):
        @pl.when(x == z)
        def _():
            arrived(Dn.at[y, c, :, pl.ds(0, (1 + late) * dcols)], d0_sem.at[late])

    lo, hi = pl.ds(0, dcut), pl.ds(dcut, drows - dcut)
    cuts = (lo, hi)

    def D1S(i):
        r = Dn.at[y, c, :, piece_cols(i)]

        @pl.when(z == x)
        def _():
            for d in (0, 1):
                begin(r, out_sem.at[5], d_sem.at[0, i], near[0][d])

        if i == 0:
            sent(Dn.at[0:2, c], out_sem.at[5], z == x)

    def D1F(i):
        for d in (0, 1):
            here = z == ring(x, 1 + 2 * d)

            @pl.when(here)
            def _():
                arrived(Dn.at[y, c, :, piece_cols(i)], d_sem.at[0, i])
                begin(Dn.at[y, c, cuts[d], piece_cols(i)], out_sem.at[6], d_sem.at[1, i], near[0][d])

            if i == 0:
                sent(Dn.at[y, c, cuts[d]], out_sem.at[6], here)

    def D1E(i):
        @pl.when(z == ring(x, 2))
        def _():
            arrived(Dn.at[y, c, :, piece_cols(i)], d_sem.at[1, i])

    def D2S(i):
        for d in (0, 1):
            begin(Dn.at[y, c, :, piece_cols(i)], out_sem.at[7], d_sem.at[2, i], near[1][d])
        if i == 0:
            sent(Dn.at[0:2, c], out_sem.at[7])

    def D2F(i):
        arrived(Dn.at[0:2, c, :, piece_cols(i)], d_sem.at[2, i])
        for d in (0, 1):
            begin(Dn.at[ring(y, 3 - 2 * d), c, cuts[d], piece_cols(i)], out_sem.at[8], d_sem.at[3, i], near[1][d])
        if i == 0:
            sent(Dn.at[y, c], out_sem.at[8])

    def D2E(i):
        arrived(Dn.at[y, c, :, piece_cols(i)], d_sem.at[3, i])
        begin(Dn.at[:, c, :, piece_cols(i)], out_sem.at[9], d_sem.at[4, i], sibling)
        if i == 0:
            sent(Dn.at[:, c], out_sem.at[9])

    def SH(i):
        arrived(Dn.at[:, 1 - c, :, piece_cols(i)], d_sem.at[4, i])
        off, p = OFFS[i]
        if off == 0:
            return
        d = (off - 1) // 2
        cols = piece_cols(i)
        hw = PIECE // 2
        if off != 2:
            arrived(R2.at[p, d], r2_sem.at[p, d])

        def body(t, _):
            at_rows = pl.ds(pl.multiple_of(t * TILE, TILE), TILE)
            w = Dn[:, :, :, cols].reshape(-1, PIECE)
            v = jnp.dot(H[at_rows, :], w, preferred_element_type=f32)
            if off == 2:
                v = v.astype(bf16)
                S2[p, 0, at_rows, :] = v[:, hw:]
                S2[p, 1, at_rows, :] = v[:, :hw]
                for e in (0, 1):
                    copy(S2.at[p, e, at_rows, :], R2.at[p, e, at_rows, :],
                         out_sem.at[10], r2_sem.at[p, e], xnear[e]).start()
                return 0
            plain, added = pl.ds(d * hw, hw), pl.ds((1 - d) * hw, hw)
            to = S1.at[d] if p == 0 else (Tp, Tm)[d]
            to[at_rows, plain] = v[:, d * hw:(d + 1) * hw].astype(bf16)
            to[at_rows, added] = (
                v[:, (1 - d) * hw:(2 - d) * hw] + R2[p, d, at_rows, :].astype(f32)).astype(bf16)
            if p == 0:
                copy(S1.at[d, at_rows, :], R1.at[d, at_rows, :], out_sem.at[11], r1_sem.at[0], xnear[d]).start()
            return 0

        lax.fori_loop(0, H.shape[0] // TILE, body, 0)
        if i == 0:
            sent(S2, out_sem.at[10])
            sent(S1, out_sem.at[11])

    def NORM(t):
        if t == 0:
            loads[4].wait()
        step = 128
        count = X.shape[0] // 3 // step

        def body(i, _):
            at_rows = pl.ds(pl.multiple_of((t * count + i) * step, step), step)
            v = X[at_rows, :].astype(f32)
            m = jnp.mean(v * v, axis=-1, keepdims=True)
            X[at_rows, :] = (v * lax.rsqrt(m + eps_norm)).astype(bf16)
            return 0

        lax.fori_loop(0, count, body, 0)

    does = {f.__name__: f for f in (P1S, P1F, P1E, P2S, P2F, P2E, HID, NORM, D0S, D0, D1S, D1F, D1E, D2S, D2F, D2E, SH)}
    for word in ORDER:
        name, *numbers = word.split(".")
        does[name](*map(int, numbers))
    arrived(R1, r1_sem.at[0])
    for cond, d in drain:
        if cond is None:
            d.wait_send()
        else:
            pl.when(cond)(d.wait_send)


def write_out(W, Dn, H, R1, g_out, u_out, d_out, done, own, sem):
    x = lax.axis_index("tp")
    ff, width = d_out.shape
    dcols = width // RING
    copies = []
    for src, out in ((W.at[0], g_out), (W.at[1], u_out), (Dn, d_out)):
        n = out.shape[0] // 4
        for i in range(4):
            r = pl.ds(i * n, n)
            copies.append(pltpu.make_async_copy(src.at[r], out.at[r], sem.at[len(copies)]))
    for cp in copies:
        cp.start()

    def body(t, _):
        at_rows = pl.ds(pl.multiple_of(t * TILE, TILE), TILE)
        w = Dn[:, pl.ds(pl.multiple_of(x * dcols, dcols), dcols)]
        v = jnp.dot(H[at_rows, :], w, preferred_element_type=f32)
        v0 = v[:, :PIECE] + R1[0, at_rows, :].astype(f32) + R1[1, at_rows, :].astype(f32)
        done[at_rows, :] = v0.astype(bf16)
        own[at_rows, :] = v[:, PIECE:]
        return 0

    lax.fori_loop(0, H.shape[0] // TILE, body, 0)
    for cp in copies:
        cp.wait()


def add_last(done, own, up, down, m_out, last, sem):
    copies = [pltpu.make_async_copy(done, m_out.at[:, pl.ds(0, PIECE)], sem.at[0]),
              pltpu.make_async_copy(last, m_out.at[:, pl.ds(PIECE, PIECE)], sem.at[1])]
    copies[0].start()
    last[...] = (own[...] + up[...].astype(f32) + down[...].astype(f32)).astype(bf16)
    copies[1].start()
    for cp in copies:
        cp.wait()


def on_device(tokens, norm_gain, gate_weight, up_weight, down_weight):
    toks, width = tokens.shape
    rows, ff = gate_weight.shape
    drows, dcols = down_weight.shape
    hbm = pl.BlockSpec(memory_space=pltpu.HBM)
    vmem = pl.BlockSpec(memory_space=pltpu.VMEM)
    dma = pltpu.SemaphoreType.DMA
    half_piece = PIECE // 2
    W, Dn, H, R1, Tp, Tm = pl.pallas_call(
        kernel,
        out_shape=(
            pltpu.VMEM((2, RING, RING, 2, rows, ff), bf16),
            pltpu.VMEM((RING, 2, drows, width), bf16),
            pltpu.VMEM((toks, ff), bf16),
            pltpu.VMEM((2, toks, PIECE), bf16),
            pltpu.VMEM((toks, PIECE), bf16),
            pltpu.VMEM((toks, PIECE), bf16),
        ),
        in_specs=[hbm] * 5,
        out_specs=(vmem,) * 6,
        scratch_shapes=[
            pltpu.VMEM((toks, width), bf16),
            pltpu.VMEM((rows, ff), f32),
            pltpu.VMEM((rows, ff), f32),
            pltpu.VMEM((drows, dcols), f32),
            pltpu.VMEM((drows, dcols), bf16),
            pltpu.VMEM((1, rows), f32),
            pltpu.VMEM((2, 2, toks, half_piece), bf16),
            pltpu.VMEM((2, toks, PIECE), bf16),
            pltpu.VMEM((2, 2, toks, half_piece), bf16),
            dma((5,)),
            dma((12,)),
            dma((2, NCH)),
            dma((NCH, 4)),
            dma((2,)),
            dma((5, NP)),
            dma((2, 2)),
            dma((1,)),
        ],
        compiler_params=pltpu.CompilerParams(
            collective_id=0, has_side_effects=True, vmem_limit_bytes=45_800_000),
    )(tokens, norm_gain.reshape(1, rows), gate_weight, up_weight, down_weight)
    up = lax.ppermute(Tp, "tp", [(i, (i + 1) % RING) for i in range(RING)])
    down = lax.ppermute(Tm, "tp", [(i, (i + RING - 1) % RING) for i in range(RING)])
    g_out, u_out, d_out, done, own = pl.pallas_call(
        write_out,
        out_shape=(
            jax.ShapeDtypeStruct((width, ff), bf16),
            jax.ShapeDtypeStruct((width, ff), bf16),
            jax.ShapeDtypeStruct((ff, width), bf16),
            pltpu.VMEM((toks, PIECE), bf16),
            pltpu.VMEM((toks, PIECE), f32),
        ),
        in_specs=[vmem] * 4,
        out_specs=(hbm,) * 3 + (vmem,) * 2,
        scratch_shapes=[dma((12,))],
        cost_estimate=pl.CostEstimate(flops=6 * 10**9, bytes_accessed=18 * 10**6, transcendentals=0),
        compiler_params=pltpu.CompilerParams(vmem_limit_bytes=12 * 2**20),
    )(W.reshape(2, width, ff), Dn.reshape(ff, width), H, R1)
    mixed = pl.pallas_call(
        add_last,
        out_shape=jax.ShapeDtypeStruct((toks, dcols), bf16),
        in_specs=[vmem] * 4,
        out_specs=hbm,
        scratch_shapes=[pltpu.VMEM((toks, PIECE), bf16), dma((2,))],
        compiler_params=pltpu.CompilerParams(vmem_limit_bytes=8 * 2**20),
    )(done, own, up, down)
    return g_out, u_out, d_out, mixed


def solution(mesh):
    in_specs = (P("fs", None), P("fs"), P("fs", "tp"), P("fs", "tp"), P("fs", "tp"))
    out_specs = (P(None, "tp"), P(None, "tp"), P("tp", None), P("fs", "tp"))
    return jax.shard_map(
        on_device, mesh=mesh, in_specs=in_specs, out_specs=out_specs, check_vma=False
    )
```

```python
import jax
import jax.numpy as jnp
from jax import lax
from jax.experimental import pallas as pl
from jax.experimental.pallas import tpu as pltpu
from jax.sharding import PartitionSpec as P

MESH = pl.DeviceIdType.MESH
bf16, f32 = jnp.bfloat16, jnp.float32
eps_norm = 1e-06
RING = 4
CHUNKS = ((0, 256), (256, 256), (512, 256), (768, 256), (1024, 256), (1280, 128))
NCH = len(CHUNKS)
PARTS = 2
PIECE = 256
OFFS = ((2, 0), (2, 1), (1, 0), (3, 0), (1, 1), (3, 1), (0, 0), (0, 1))
NP = len(OFFS)
TILE = 256
ORDER = (
    "P1S.0", "P1S.1", "NORM.0", "D0S.0", "P1S.2", "P2S.0.0", "P1S.3", "P1S.4", "P1F.1", "P1F.0", "P2S.5.0",
    "P2S.1.1", "P2S.1.0", "P1S.5", "P1F.3", "P1F.4", "P2S.1.3", "P2S.4.1", "D0.0", "P2S.0.3", "D1S.0",
    "P1F.5", "P1E.1", "P1E.4", "D0S.1", "P2S.3.0", "P2S.4.3", "NORM.1", "P2S.1.2", "P2S.4.0", "P2S.5.3",
    "P2S.4.2", "P1E.0", "P2S.0.2", "P1E.5", "P1E.3", "P2S.5.1", "P1F.2", "P2S.3.1", "P2S.5.2", "D0.1",
    "P2S.2.0", "D1F.0", "D1S.1", "P2F.4", "P1E.2", "P2S.0.1", "P2F.5", "P2S.3.3", "NORM.2", "P2F.1",
    "D1F.1", "P2S.2.1", "P2S.2.3", "P2E.4", "P2S.2.2", "P2E.5", "P2F.0", "D1E.0", "D2S.0", "P2S.3.2",
    "HID.4.0", "HID.5.0", "D1S.2", "P2E.1", "HID.4.1", "D1E.1", "D2S.1", "P2F.2", "HID.1.0", "P2E.0",
    "D2F.0", "HID.5.1", "D1S.3", "P2F.3", "D1F.2", "D1S.4", "D1S.5", "HID.0.0", "D2F.1", "P2E.2", "HID.1.1",
    "HID.0.1", "D1S.6", "D1F.3", "D1E.2", "D2S.2", "D2E.0", "HID.2.0", "P2E.3", "HID.2.1", "D1E.3", "D2S.3",
    "D2E.1", "D1F.4", "D1S.7", "HID.3.0", "SHA.0", "HID.3.1", "D2F.2", "D1F.5", "SHA.1", "D1E.4", "D2F.3",
    "D2S.4", "D1F.6", "SH.1", "D2E.2", "D1F.7", "D1E.5", "D2S.5", "D2E.3", "D1E.6", "D2S.6", "SH.2",
    "D1E.7", "D2S.7", "SH.3", "D2F.4", "D2F.5", "D2F.6", "D2F.7", "D2E.4", "D2E.5", "D2E.6", "D2E.7",
    "SH.4", "SH.5", "SH.6", "SH.7",
)


def ring(v, k):
    return lax.rem(v + k, RING)


def kernel(tok, gain, gw, uw, dw, W, Dn, H, R1, Tp, Tm, X, gs, us, ds, dst, gv, S2, S1, R2,
           in_sem, out_sem, sib_sem, gu_sem, d0_sem, d_sem, r2_sem, r1_sem):
    x = lax.axis_index("tp")
    f = lax.axis_index("fs")
    c = lax.rem(f, 2)
    y = lax.rem(lax.div(f, 2), RING)
    z = lax.div(f, 2 * RING)
    rows, half = gs.shape[0], gs.shape[0] // 2
    drows, dcols = ds.shape
    dcut = 96

    def at(zz, yy, cc):
        return {"fs": (zz * RING + yy) * 2 + cc}

    zp, zm, yp, ym = ring(z, 1), ring(z, 3), ring(y, 1), ring(y, 3)
    near = ((at(zp, y, c), at(zm, y, c)), (at(z, yp, c), at(z, ym, c)))
    sibling = at(z, y, 1 - c)
    xnear = ({"tp": ring(x, 1)}, {"tp": ring(x, 3)})

    drain = []

    def copy(src, dst, ss, rs, dev):
        return pltpu.make_async_remote_copy(
            src_ref=src, dst_ref=dst, send_sem=ss, recv_sem=rs, device_id=dev, device_id_type=MESH)

    def begin(src, ss, rs, dev):
        copy(src, src, ss, rs, dev).start()

    def arrived(view, rs):
        copy(view, view, out_sem.at[0], rs, sibling).wait_recv()

    def sent(view, ss, cond=None):
        drain.append((cond, copy(view, view, ss, ss, sibling)))

    loads = [pltpu.make_async_copy(s, d, in_sem.at[i])
             for i, (s, d) in enumerate(((gain, gv), (gw, gs), (uw, us), (dw, ds), (tok, X)))]
    for l in loads:
        l.start()
    barrier = pltpu.get_barrier_semaphore()
    greet = [*near[0], *near[1], sibling, {"tp": ring(x, 1)}, {"tp": ring(x, 2)}, {"tp": ring(x, 3)}]
    for dev in greet:
        pl.semaphore_signal(barrier, inc=1, device_id=dev, device_id_type=MESH)

    for l in loads[:3]:
        l.wait()
    eye = lax.broadcasted_iota(jnp.int32, (rows, rows), 0) == lax.broadcasted_iota(jnp.int32, (rows, rows), 1)
    column = jnp.sum(jnp.where(eye, gv[...], 0.0), axis=1, keepdims=True)
    W[0, z, y, c] = (gs[...] * column).astype(bf16)
    W[1, z, y, c] = (us[...] * column).astype(bf16)
    pl.semaphore_wait(barrier, len(greet))

    def cols_of(k):
        return pl.ds(*CHUNKS[k])

    def region(a, first, second, part, k):
        zz, yy = (ring(z, first), ring(y, second)) if a == 0 else (ring(z, second), ring(y, first))
        lead = slice(None) if part is None else part
        return W.at[lead, zz, yy, c, pl.ds(a * half, half), cols_of(k)]

    def line(a, second, core, k, part=None):
        lead = slice(None) if part is None else part
        if a == 0:
            return W.at[lead, :, ring(y, second), core, pl.ds(0, half), cols_of(k)]
        return W.at[lead, ring(z, second), :, core, pl.ds(half, half), cols_of(k)]

    def P1S(k):
        for d in (0, 1):
            for a in (0, 1):
                begin(region(a, 0, 0, None, k), out_sem.at[0], gu_sem.at[k, 0], near[a][d])
        if k == 0:
            sent(W.at[:, 0, 0], out_sem.at[0])

    def P1F(k):
        arrived(W.at[:, 0, 0, :, :, cols_of(k)], gu_sem.at[k, 0])
        for d in (0, 1):
            for a in (0, 1):
                begin(region(a, 3 - 2 * d, 0, d, k), out_sem.at[1], gu_sem.at[k, 1], near[a][d])
        if k == 0:
            sent(W.at[0, 0, 0], out_sem.at[1])

    def P1E(k):
        arrived(W.at[0, 0, 0, :, :, cols_of(k)], gu_sem.at[k, 1])

    def P2S(k, j):
        for d in (0, 1):
            for a in (0, 1):
                begin(region(a, j, 0, None, k), out_sem.at[2], gu_sem.at[k, 2], near[1 - a][d])
        if k == 0 and j == 0:
            sent(W.at[:, :, 0], out_sem.at[2])

    def sib(k, second):
        for a in (0, 1):
            begin(line(a, second, c, k), sib_sem.at[0, k], sib_sem.at[1, k], sibling)

    def P2F(k):
        arrived(W.at[:, :, 0, :, :, cols_of(k)], gu_sem.at[k, 2])
        for d in (0, 1):
            for a in (0, 1):
                begin(line(a, 3 - 2 * d, c, k, d), out_sem.at[3], gu_sem.at[k, 3], near[1 - a][d])
        if k == 0:
            sent(W.at[0, :, 0], out_sem.at[3])
        for second in (0, 1, 3):
            sib(k, second)

    def P2E(k):
        arrived(W.at[0, :, 0, :, :, cols_of(k)], gu_sem.at[k, 3])
        sib(k, 2)
        sent(W.at[:, :, :, c, :, cols_of(k)], sib_sem.at[0, k])

    def HID(k, t):
        if t == 0:
            arrived(W.at[:, :, :, 1 - c, :, cols_of(k)], sib_sem.at[1, k])
        start, width = CHUNKS[k]
        tile = X.shape[0] // PARTS
        at_rows = pl.ds(t * tile, tile)
        cols = pl.ds(start, width)
        w = jnp.concatenate([W[0, :, :, :, :, cols].reshape(-1, width), W[1, :, :, :, :, cols].reshape(-1, width)], axis=1)
        v = jnp.dot(X[at_rows, :], w, preferred_element_type=f32)
        g, u = v[:, :width], v[:, width:]
        H[at_rows, cols] = (g / (1.0 + jnp.exp(-g)) * u).astype(bf16)

    def place(q):
        return pl.multiple_of(q * dcols, dcols)

    def piece_cols(i):
        off, p = OFFS[i]
        return pl.ds(pl.multiple_of(ring(x, off) * dcols + p * PIECE, PIECE), PIECE)

    def D0S(late):
        mine = pl.ds(place(x), dcols)
        if not late:
            loads[3].wait()
            rounded = ds[...].astype(bf16)
            dst[...] = rounded

            @pl.when(x == z)
            def _():
                Dn[y, c, :, mine] = rounded

        go = (z == ring(x, 1)) | (z == ring(x, 3)) if late else z == ring(x, 2)
        pl.when(go)(copy(dst, Dn.at[y, c, :, mine], out_sem.at[4], d0_sem.at[late], {"tp": z}).start)
        if late:
            sent(dst, out_sem.at[4], z != x)

    def D0(late):
        @pl.when(x == z)
        def _():
            arrived(Dn.at[y, c, :, pl.ds(0, (1 + late) * dcols)], d0_sem.at[late])

    lo, hi = pl.ds(0, dcut), pl.ds(dcut, drows - dcut)
    cuts = (lo, hi)

    def D1S(i):
        r = Dn.at[y, c, :, piece_cols(i)]

        @pl.when(z == x)
        def _():
            for d in (0, 1):
                begin(r, out_sem.at[5], d_sem.at[0, i], near[0][d])

        if i == 0:
            sent(Dn.at[0:2, c], out_sem.at[5], z == x)

    def D1F(i):
        for d in (0, 1):
            here = z == ring(x, 1 + 2 * d)

            @pl.when(here)
            def _():
                arrived(Dn.at[y, c, :, piece_cols(i)], d_sem.at[0, i])
                begin(Dn.at[y, c, cuts[d], piece_cols(i)], out_sem.at[6], d_sem.at[1, i], near[0][d])

            if i == 0:
                sent(Dn.at[y, c, cuts[d]], out_sem.at[6], here)

    def D1E(i):
        @pl.when(z == ring(x, 2))
        def _():
            arrived(Dn.at[y, c, :, piece_cols(i)], d_sem.at[1, i])

    def D2S(i):
        for d in (0, 1):
            begin(Dn.at[y, c, :, piece_cols(i)], out_sem.at[7], d_sem.at[2, i], near[1][d])
        if i == 0:
            sent(Dn.at[0:2, c], out_sem.at[7])

    def D2F(i):
        arrived(Dn.at[0:2, c, :, piece_cols(i)], d_sem.at[2, i])
        for d in (0, 1):
            begin(Dn.at[ring(y, 3 - 2 * d), c, cuts[d], piece_cols(i)], out_sem.at[8], d_sem.at[3, i], near[1][d])
        if i == 0:
            sent(Dn.at[y, c], out_sem.at[8])

    def D2E(i):
        arrived(Dn.at[y, c, :, piece_cols(i)], d_sem.at[3, i])
        begin(Dn.at[:, c, :, piece_cols(i)], out_sem.at[9], d_sem.at[4, i], sibling)
        if i == 0:
            sent(Dn.at[:, c], out_sem.at[9])

    def SHA(t):
        SH(0, t)

    def SH(i, part=None):
        if not part:
            arrived(Dn.at[:, 1 - c, :, piece_cols(i)], d_sem.at[4, i])
        off, p = OFFS[i]
        if off == 0:
            return
        d = (off - 1) // 2
        cols = piece_cols(i)
        hw = PIECE // 2
        if off != 2:
            arrived(R2.at[p, d], r2_sem.at[p, d])

        def body(t, _):
            tile = TILE if part is None else H.shape[0] // PARTS
            at_rows = pl.ds(pl.multiple_of(t * tile, tile), tile)
            w = Dn[:, :, :, cols].reshape(-1, PIECE)
            v = jnp.dot(H[at_rows, :], w, preferred_element_type=f32)
            if off == 2:
                v = v.astype(bf16)
                S2[p, 0, at_rows, :] = v[:, hw:]
                S2[p, 1, at_rows, :] = v[:, :hw]
                for e in (0, 1):
                    copy(S2.at[p, e, at_rows, :], R2.at[p, e, at_rows, :],
                         out_sem.at[10], r2_sem.at[p, e], xnear[e]).start()
                return 0
            plain, added = pl.ds(d * hw, hw), pl.ds((1 - d) * hw, hw)
            to = S1.at[d] if p == 0 else (Tp, Tm)[d]
            to[at_rows, plain] = v[:, d * hw:(d + 1) * hw].astype(bf16)
            to[at_rows, added] = (
                v[:, (1 - d) * hw:(2 - d) * hw] + R2[p, d, at_rows, :].astype(f32)).astype(bf16)
            if p == 0:
                copy(S1.at[d, at_rows, :], R1.at[d, at_rows, :], out_sem.at[11], r1_sem.at[0], xnear[d]).start()
            return 0

        if part is None:
            lax.fori_loop(0, H.shape[0] // TILE, body, 0)
        else:
            body(part, 0)
        if i == 1:
            sent(S2, out_sem.at[10])
            sent(S1, out_sem.at[11])

    def NORM(t):
        if t == 0:
            loads[4].wait()
        step = 128
        count = X.shape[0] // 3 // step

        def body(i, _):
            at_rows = pl.ds(pl.multiple_of((t * count + i) * step, step), step)
            v = X[at_rows, :].astype(f32)
            m = jnp.mean(v * v, axis=-1, keepdims=True)
            X[at_rows, :] = (v * lax.rsqrt(m + eps_norm)).astype(bf16)
            return 0

        lax.fori_loop(0, count, body, 0)

    does = {f.__name__: f for f in (P1S, P1F, P1E, P2S, P2F, P2E, HID, NORM, D0S, D0, D1S, D1F, D1E, D2S, D2F, D2E, SH, SHA)}
    for word in ORDER:
        name, *numbers = word.split(".")
        does[name](*map(int, numbers))
    arrived(R1, r1_sem.at[0])
    for cond, d in drain:
        if cond is None:
            d.wait_send()
        else:
            pl.when(cond)(d.wait_send)


def write_out(W, Dn, H, R1, g_out, u_out, d_out, done, own, sem):
    x = lax.axis_index("tp")
    ff, width = d_out.shape
    dcols = width // RING
    copies = []
    for src, out in ((W.at[0], g_out), (W.at[1], u_out), (Dn, d_out)):
        n = out.shape[0] // 4
        for i in range(4):
            r = pl.ds(i * n, n)
            copies.append(pltpu.make_async_copy(src.at[r], out.at[r], sem.at[len(copies)]))
    for cp in copies:
        cp.start()

    def body(t, _):
        at_rows = pl.ds(pl.multiple_of(t * TILE, TILE), TILE)
        w = Dn[:, pl.ds(pl.multiple_of(x * dcols, dcols), dcols)]
        v = jnp.dot(H[at_rows, :], w, preferred_element_type=f32)
        v0 = v[:, :PIECE] + R1[0, at_rows, :].astype(f32) + R1[1, at_rows, :].astype(f32)
        done[at_rows, :] = v0.astype(bf16)
        own[at_rows, :] = v[:, PIECE:]
        return 0

    lax.fori_loop(0, H.shape[0] // TILE, body, 0)
    for cp in copies:
        cp.wait()


def add_last(done, own, up, down, m_out, last, sem):
    copies = [pltpu.make_async_copy(done, m_out.at[:, pl.ds(0, PIECE)], sem.at[0]),
              pltpu.make_async_copy(last, m_out.at[:, pl.ds(PIECE, PIECE)], sem.at[1])]
    copies[0].start()
    last[...] = (own[...] + up[...].astype(f32) + down[...].astype(f32)).astype(bf16)
    copies[1].start()
    for cp in copies:
        cp.wait()


def on_device(tokens, norm_gain, gate_weight, up_weight, down_weight):
    toks, width = tokens.shape
    rows, ff = gate_weight.shape
    drows, dcols = down_weight.shape
    hbm = pl.BlockSpec(memory_space=pltpu.HBM)
    vmem = pl.BlockSpec(memory_space=pltpu.VMEM)
    dma = pltpu.SemaphoreType.DMA
    half_piece = PIECE // 2
    W, Dn, H, R1, Tp, Tm = pl.pallas_call(
        kernel,
        out_shape=(
            pltpu.VMEM((2, RING, RING, 2, rows, ff), bf16),
            pltpu.VMEM((RING, 2, drows, width), bf16),
            pltpu.VMEM((toks, ff), bf16),
            pltpu.VMEM((2, toks, PIECE), bf16),
            pltpu.VMEM((toks, PIECE), bf16),
            pltpu.VMEM((toks, PIECE), bf16),
        ),
        in_specs=[hbm] * 5,
        out_specs=(vmem,) * 6,
        scratch_shapes=[
            pltpu.VMEM((toks, width), bf16),
            pltpu.VMEM((rows, ff), f32),
            pltpu.VMEM((rows, ff), f32),
            pltpu.VMEM((drows, dcols), f32),
            pltpu.VMEM((drows, dcols), bf16),
            pltpu.VMEM((1, rows), f32),
            pltpu.VMEM((2, 2, toks, half_piece), bf16),
            pltpu.VMEM((2, toks, PIECE), bf16),
            pltpu.VMEM((2, 2, toks, half_piece), bf16),
            dma((5,)),
            dma((12,)),
            dma((2, NCH)),
            dma((NCH, 4)),
            dma((2,)),
            dma((5, NP)),
            dma((2, 2)),
            dma((1,)),
        ],
        compiler_params=pltpu.CompilerParams(
            collective_id=0, has_side_effects=True, vmem_limit_bytes=45_800_000),
    )(tokens, norm_gain.reshape(1, rows), gate_weight, up_weight, down_weight)
    up = lax.ppermute(Tp, "tp", [(i, (i + 1) % RING) for i in range(RING)])
    down = lax.ppermute(Tm, "tp", [(i, (i + RING - 1) % RING) for i in range(RING)])
    g_out, u_out, d_out, done, own = pl.pallas_call(
        write_out,
        out_shape=(
            jax.ShapeDtypeStruct((width, ff), bf16),
            jax.ShapeDtypeStruct((width, ff), bf16),
            jax.ShapeDtypeStruct((ff, width), bf16),
            pltpu.VMEM((toks, PIECE), bf16),
            pltpu.VMEM((toks, PIECE), f32),
        ),
        in_specs=[vmem] * 4,
        out_specs=(hbm,) * 3 + (vmem,) * 2,
        scratch_shapes=[dma((12,))],
        cost_estimate=pl.CostEstimate(flops=6 * 10**9, bytes_accessed=18 * 10**6, transcendentals=0),
        compiler_params=pltpu.CompilerParams(vmem_limit_bytes=12 * 2**20),
    )(W.reshape(2, width, ff), Dn.reshape(ff, width), H, R1)
    mixed = pl.pallas_call(
        add_last,
        out_shape=jax.ShapeDtypeStruct((toks, dcols), bf16),
        in_specs=[vmem] * 4,
        out_specs=hbm,
        scratch_shapes=[pltpu.VMEM((toks, PIECE), bf16), dma((2,))],
        compiler_params=pltpu.CompilerParams(vmem_limit_bytes=8 * 2**20),
    )(done, own, up, down)
    return g_out, u_out, d_out, mixed


def solution(mesh):
    in_specs = (P("fs", None), P("fs"), P("fs", "tp"), P("fs", "tp"), P("fs", "tp"))
    out_specs = (P(None, "tp"), P(None, "tp"), P("tp", None), P("fs", "tp"))
    return jax.shard_map(
        on_device, mesh=mesh, in_specs=in_specs, out_specs=out_specs, check_vma=False
    )
```

```python
import jax
import jax.numpy as jnp
from jax import lax
from jax.experimental import pallas as pl
from jax.experimental.pallas import tpu as pltpu
from jax.sharding import PartitionSpec as P

MESH = pl.DeviceIdType.MESH
bf16, f32 = jnp.bfloat16, jnp.float32
eps_norm = 1e-06
RING = 4
CHUNKS = ((0, 256), (256, 256), (512, 256), (768, 256), (1024, 256), (1280, 128))
NCH = len(CHUNKS)
PARTS = 2
PIECE = 256
OFFS = ((2, 0), (2, 1), (1, 0), (3, 0), (1, 1), (3, 1), (0, 0), (0, 1))
NP = len(OFFS)
TILE = 256
ORDER = (
    "P1S.0", "P1S.1", "NORM.0", "D0S.0", "P1S.2", "P2S.0.0", "P1S.3", "P1S.4", "P1F.1", "P1F.0", "P2S.5.0",
    "P2S.1.1", "P2S.1.0", "P1S.5", "P1F.3", "P1F.4", "P2S.1.3", "P2S.4.1", "D0.0", "P2S.0.3", "D1S.0",
    "P1F.5", "P1E.1", "P1E.4", "D0S.1", "P2S.3.0", "P2S.4.3", "NORM.1", "P2S.1.2", "P2S.4.0", "P2S.5.3",
    "P2S.4.2", "P1E.0", "P2S.0.2", "P1E.5", "P1E.3", "P2S.5.1", "P1F.2", "P2S.3.1", "P2S.5.2", "D0.1",
    "P2S.2.0", "D1F.0", "D1S.1", "P2F.4", "P1E.2", "P2S.0.1", "P2F.5", "P2S.3.3", "NORM.2", "P2F.1",
    "D1F.1", "P2S.2.1", "P2S.2.3", "P2E.4", "P2S.2.2", "P2E.5", "P2F.0", "D1E.0", "D2S.0", "P2S.3.2",
    "HID.4.0", "HID.5.0", "D1S.2", "P2E.1", "HID.4.1", "D1E.1", "D2S.1", "P2F.2", "HID.1.0", "P2E.0",
    "D2F.0", "HID.5.1", "D1S.3", "P2F.3", "D1F.2", "D1S.4", "D1S.5", "HID.0.0", "D2F.1", "P2E.2", "HID.1.1",
    "HID.0.1", "D1S.6", "D1F.3", "D1E.2", "D2S.2", "D2E.0", "HID.2.0", "P2E.3", "HID.2.1", "D1E.3", "D2S.3",
    "D2E.1", "D1F.4", "D1S.7", "HID.3.0", "SHA.0", "HID.3.1", "D2F.2", "D1F.5", "SHA.1", "D1E.4", "D2F.3",
    "D2S.4", "D1F.6", "SH.1", "D2E.2", "D1F.7", "D1E.5", "D2S.5", "D2E.3", "D1E.6", "D2S.6", "SH.2",
    "D1E.7", "D2S.7", "SH.3", "D2F.4", "D2F.5", "D2F.6", "D2F.7", "D2E.4", "D2E.5", "D2E.6", "D2E.7",
    "SH.4", "SH.5", "SH.6", "SH.7",
)


def ring(v, k):
    return lax.rem(v + k, RING)


def kernel(tok, gain, gw, uw, dw, W, Dn, H, R1, Tp, Tm, X, gs, us, ds, dst, gv, S2, S1, R2,
           in_sem, out_sem, sib_sem, gu_sem, d0_sem, d_sem, r2_sem, r1_sem):
    x = lax.axis_index("tp")
    f = lax.axis_index("fs")
    c = lax.rem(f, 2)
    y = lax.rem(lax.div(f, 2), RING)
    z = lax.div(f, 2 * RING)
    rows, half = gs.shape[0], gs.shape[0] // 2
    drows, dcols = ds.shape
    dcut = 96

    def at(zz, yy, cc):
        return {"fs": (zz * RING + yy) * 2 + cc}

    zp, zm, yp, ym = ring(z, 1), ring(z, 3), ring(y, 1), ring(y, 3)
    near = ((at(zp, y, c), at(zm, y, c)), (at(z, yp, c), at(z, ym, c)))
    sibling = at(z, y, 1 - c)
    xnear = ({"tp": ring(x, 1)}, {"tp": ring(x, 3)})

    drain = []

    def copy(src, dst, ss, rs, dev):
        return pltpu.make_async_remote_copy(
            src_ref=src, dst_ref=dst, send_sem=ss, recv_sem=rs, device_id=dev, device_id_type=MESH)

    def begin(src, ss, rs, dev):
        copy(src, src, ss, rs, dev).start()

    def arrived(view, rs):
        copy(view, view, out_sem.at[0], rs, sibling).wait_recv()

    def sent(view, ss, cond=None):
        drain.append((cond, copy(view, view, ss, ss, sibling)))

    loads = [pltpu.make_async_copy(s, d, in_sem.at[i])
             for i, (s, d) in enumerate(((gain, gv), (gw, gs), (uw, us), (dw, ds), (tok, X)))]
    for l in loads:
        l.start()
    barrier = pltpu.get_barrier_semaphore()
    greet = [*near[0], *near[1], sibling, {"tp": ring(x, 1)}, {"tp": ring(x, 2)}, {"tp": ring(x, 3)}]
    for dev in greet:
        pl.semaphore_signal(barrier, inc=1, device_id=dev, device_id_type=MESH)

    for l in loads[:3]:
        l.wait()
    eye = lax.broadcasted_iota(jnp.int32, (rows, rows), 0) == lax.broadcasted_iota(jnp.int32, (rows, rows), 1)
    column = jnp.sum(jnp.where(eye, gv[...], 0.0), axis=1, keepdims=True)
    W[0, z, y, c] = (gs[...] * column).astype(bf16)
    W[1, z, y, c] = (us[...] * column).astype(bf16)
    pl.semaphore_wait(barrier, len(greet))

    def cols_of(k):
        return pl.ds(*CHUNKS[k])

    def region(a, first, second, part, k):
        zz, yy = (ring(z, first), ring(y, second)) if a == 0 else (ring(z, second), ring(y, first))
        lead = slice(None) if part is None else part
        return W.at[lead, zz, yy, c, pl.ds(a * half, half), cols_of(k)]

    def line(a, second, core, k, part=None):
        lead = slice(None) if part is None else part
        if a == 0:
            return W.at[lead, :, ring(y, second), core, pl.ds(0, half), cols_of(k)]
        return W.at[lead, ring(z, second), :, core, pl.ds(half, half), cols_of(k)]

    def P1S(k):
        for d in (0, 1):
            for a in (0, 1):
                begin(region(a, 0, 0, None, k), out_sem.at[0], gu_sem.at[k, 0], near[a][d])
        if k == 0:
            sent(W.at[:, 0, 0], out_sem.at[0])

    def P1F(k):
        arrived(W.at[:, 0, 0, :, :, cols_of(k)], gu_sem.at[k, 0])
        for d in (0, 1):
            for a in (0, 1):
                begin(region(a, 3 - 2 * d, 0, d, k), out_sem.at[1], gu_sem.at[k, 1], near[a][d])
        if k == 0:
            sent(W.at[0, 0, 0], out_sem.at[1])

    def P1E(k):
        arrived(W.at[0, 0, 0, :, :, cols_of(k)], gu_sem.at[k, 1])

    def P2S(k, j):
        for d in (0, 1):
            for a in (0, 1):
                begin(region(a, j, 0, None, k), out_sem.at[2], gu_sem.at[k, 2], near[1 - a][d])
        if k == 0 and j == 0:
            sent(W.at[:, :, 0], out_sem.at[2])

    def sib(k, second):
        for a in (0, 1):
            begin(line(a, second, c, k), sib_sem.at[0, k], sib_sem.at[1, k], sibling)

    def P2F(k):
        arrived(W.at[:, :, 0, :, :, cols_of(k)], gu_sem.at[k, 2])
        for d in (0, 1):
            for a in (0, 1):
                begin(line(a, 3 - 2 * d, c, k, d), out_sem.at[3], gu_sem.at[k, 3], near[1 - a][d])
        if k == 0:
            sent(W.at[0, :, 0], out_sem.at[3])
        for second in (0, 1, 3):
            sib(k, second)

    def P2E(k):
        arrived(W.at[0, :, 0, :, :, cols_of(k)], gu_sem.at[k, 3])
        sib(k, 2)
        sent(W.at[:, :, :, c, :, cols_of(k)], sib_sem.at[0, k])

    def HID(k, t):
        if t == 0:
            arrived(W.at[:, :, :, 1 - c, :, cols_of(k)], sib_sem.at[1, k])
        start, width = CHUNKS[k]
        tile = X.shape[0] // PARTS
        at_rows = pl.ds(t * tile, tile)
        cols = pl.ds(start, width)
        w = jnp.concatenate([W[0, :, :, :, :, cols].reshape(-1, width), W[1, :, :, :, :, cols].reshape(-1, width)], axis=1)
        v = jnp.dot(X[at_rows, :], w, preferred_element_type=f32)
        g, u = v[:, :width], v[:, width:]
        H[at_rows, cols] = (g / (1.0 + jnp.exp(-g)) * u).astype(bf16)

    def place(q):
        return pl.multiple_of(q * dcols, dcols)

    def piece_cols(i):
        off, p = OFFS[i]
        return pl.ds(pl.multiple_of(ring(x, off) * dcols + p * PIECE, PIECE), PIECE)

    def D0S(late):
        mine = pl.ds(place(x), dcols)
        if not late:
            loads[3].wait()
            rounded = ds[...].astype(bf16)
            dst[...] = rounded

            @pl.when(x == z)
            def _():
                Dn[y, c, :, mine] = rounded

        go = (z == ring(x, 1)) | (z == ring(x, 3)) if late else z == ring(x, 2)
        pl.when(go)(copy(dst, Dn.at[y, c, :, mine], out_sem.at[4], d0_sem.at[late], {"tp": z}).start)
        if late:
            sent(dst, out_sem.at[4], z != x)

    def D0(late):
        @pl.when(x == z)
        def _():
            arrived(Dn.at[y, c, :, pl.ds(0, (1 + late) * dcols)], d0_sem.at[late])

    lo, hi = pl.ds(0, dcut), pl.ds(dcut, drows - dcut)
    cuts = (lo, hi)

    def D1S(i):
        r = Dn.at[y, c, :, piece_cols(i)]

        @pl.when(z == x)
        def _():
            for d in (0, 1):
                begin(r, out_sem.at[5], d_sem.at[0, i], near[0][d])

        if i == 0:
            sent(Dn.at[0:2, c], out_sem.at[5], z == x)

    def D1F(i):
        for d in (0, 1):
            here = z == ring(x, 1 + 2 * d)

            @pl.when(here)
            def _():
                arrived(Dn.at[y, c, :, piece_cols(i)], d_sem.at[0, i])
                begin(Dn.at[y, c, cuts[d], piece_cols(i)], out_sem.at[6], d_sem.at[1, i], near[0][d])

            if i == 0:
                sent(Dn.at[y, c, cuts[d]], out_sem.at[6], here)

    def D1E(i):
        @pl.when(z == ring(x, 2))
        def _():
            arrived(Dn.at[y, c, :, piece_cols(i)], d_sem.at[1, i])

    def D2S(i):
        for d in (0, 1):
            begin(Dn.at[y, c, :, piece_cols(i)], out_sem.at[7], d_sem.at[2, i], near[1][d])
        if i == 0:
            sent(Dn.at[0:2, c], out_sem.at[7])

    def D2F(i):
        arrived(Dn.at[0:2, c, :, piece_cols(i)], d_sem.at[2, i])
        for d in (0, 1):
            begin(Dn.at[ring(y, 3 - 2 * d), c, cuts[d], piece_cols(i)], out_sem.at[8], d_sem.at[3, i], near[1][d])
        if i == 0:
            sent(Dn.at[y, c], out_sem.at[8])

    def D2E(i):
        arrived(Dn.at[y, c, :, piece_cols(i)], d_sem.at[3, i])
        begin(Dn.at[:, c, :, piece_cols(i)], out_sem.at[9], d_sem.at[4, i], sibling)
        if i == 0:
            sent(Dn.at[:, c], out_sem.at[9])

    def SHA(t):
        SH(0, t)

    def SH(i, part=None):
        if not part:
            arrived(Dn.at[:, 1 - c, :, piece_cols(i)], d_sem.at[4, i])
        off, p = OFFS[i]
        if off == 0:
            return
        d = (off - 1) // 2
        cols = piece_cols(i)
        hw = PIECE // 2
        if off != 2:
            arrived(R2.at[p, d], r2_sem.at[p, d])

        def body(t, _):
            tile = TILE if part is None else H.shape[0] // PARTS
            at_rows = pl.ds(pl.multiple_of(t * tile, tile), tile)
            w = Dn[:, :, :, cols].reshape(-1, PIECE)
            v = jnp.dot(H[at_rows, :], w, preferred_element_type=f32)
            if off == 2:
                v = v.astype(bf16)
                S2[p, 0, at_rows, :] = v[:, hw:]
                S2[p, 1, at_rows, :] = v[:, :hw]
                for e in (0, 1):
                    copy(S2.at[p, e, at_rows, :], R2.at[p, e, at_rows, :],
                         out_sem.at[10], r2_sem.at[p, e], xnear[e]).start()
                return 0
            plain, added = pl.ds(d * hw, hw), pl.ds((1 - d) * hw, hw)
            to = S1.at[d] if p == 0 else (Tp, Tm)[d]
            to[at_rows, plain] = v[:, d * hw:(d + 1) * hw].astype(bf16)
            to[at_rows, added] = (
                v[:, (1 - d) * hw:(2 - d) * hw] + R2[p, d, at_rows, :].astype(f32)).astype(bf16)
            if p == 0:
                copy(S1.at[d, at_rows, :], R1.at[d, at_rows, :], out_sem.at[11], r1_sem.at[0], xnear[d]).start()
            return 0

        if part is None:
            lax.fori_loop(0, H.shape[0] // TILE, body, 0)
        else:
            body(part, 0)
        if i == 1:
            sent(S2, out_sem.at[10])
            sent(S1, out_sem.at[11])

    def NORM(t):
        if t == 0:
            loads[4].wait()
        step = 128
        count = X.shape[0] // 3 // step

        def body(i, _):
            at_rows = pl.ds(pl.multiple_of((t * count + i) * step, step), step)
            v = X[at_rows, :].astype(f32)
            m = jnp.mean(v * v, axis=-1, keepdims=True)
            X[at_rows, :] = (v * lax.rsqrt(m + eps_norm)).astype(bf16)
            return 0

        lax.fori_loop(0, count, body, 0)

    does = {f.__name__: f for f in (P1S, P1F, P1E, P2S, P2F, P2E, HID, NORM, D0S, D0, D1S, D1F, D1E, D2S, D2F, D2E, SH, SHA)}
    for word in ORDER:
        name, *numbers = word.split(".")
        does[name](*map(int, numbers))
    arrived(R1, r1_sem.at[0])
    for cond, d in drain:
        if cond is None:
            d.wait_send()
        else:
            pl.when(cond)(d.wait_send)


def write_out(W, Dn, H, R1, g_out, u_out, d_out, m_out, own, done, sem):
    x = lax.axis_index("tp")
    ff, width = d_out.shape
    dcols = width // RING
    copies = []
    for src, out in ((W.at[0], g_out), (W.at[1], u_out), (Dn, d_out)):
        n = out.shape[0] // 4
        for i in range(4):
            r = pl.ds(i * n, n)
            copies.append(pltpu.make_async_copy(src.at[r], out.at[r], sem.at[len(copies)]))
    for cp in copies:
        cp.start()

    def body(t, _):
        at_rows = pl.ds(pl.multiple_of(t * TILE, TILE), TILE)
        w = Dn[:, pl.ds(pl.multiple_of(x * dcols, dcols), dcols)]
        v = jnp.dot(H[at_rows, :], w, preferred_element_type=f32)
        v0 = v[:, :PIECE] + R1[0, at_rows, :].astype(f32) + R1[1, at_rows, :].astype(f32)
        done[at_rows, :] = v0.astype(bf16)
        own[at_rows, :] = v[:, PIECE:]
        return 0

    lax.fori_loop(0, H.shape[0] // TILE, body, 0)
    copies.append(pltpu.make_async_copy(done, m_out.at[:, pl.ds(0, PIECE)], sem.at[len(copies)]))
    copies[-1].start()
    for cp in copies:
        cp.wait()


def add_last(m_in, own, up, down, m_out, last, sem):
    copies = []
    for t in range(own.shape[0] // TILE):
        r = pl.ds(t * TILE, TILE)
        last[r, :] = (own[r, :] + up[r, :].astype(f32) + down[r, :].astype(f32)).astype(bf16)
        copies.append(pltpu.make_async_copy(last.at[r], m_out.at[r, pl.ds(PIECE, PIECE)], sem.at[t]))
        copies[-1].start()
    for cp in copies:
        cp.wait()


def on_device(tokens, norm_gain, gate_weight, up_weight, down_weight):
    toks, width = tokens.shape
    rows, ff = gate_weight.shape
    drows, dcols = down_weight.shape
    hbm = pl.BlockSpec(memory_space=pltpu.HBM)
    vmem = pl.BlockSpec(memory_space=pltpu.VMEM)
    dma = pltpu.SemaphoreType.DMA
    half_piece = PIECE // 2
    W, Dn, H, R1, Tp, Tm = pl.pallas_call(
        kernel,
        out_shape=(
            pltpu.VMEM((2, RING, RING, 2, rows, ff), bf16),
            pltpu.VMEM((RING, 2, drows, width), bf16),
            pltpu.VMEM((toks, ff), bf16),
            pltpu.VMEM((2, toks, PIECE), bf16),
            pltpu.VMEM((toks, PIECE), bf16),
            pltpu.VMEM((toks, PIECE), bf16),
        ),
        in_specs=[hbm] * 5,
        out_specs=(vmem,) * 6,
        scratch_shapes=[
            pltpu.VMEM((toks, width), bf16),
            pltpu.VMEM((rows, ff), f32),
            pltpu.VMEM((rows, ff), f32),
            pltpu.VMEM((drows, dcols), f32),
            pltpu.VMEM((drows, dcols), bf16),
            pltpu.VMEM((1, rows), f32),
            pltpu.VMEM((2, 2, toks, half_piece), bf16),
            pltpu.VMEM((2, toks, PIECE), bf16),
            pltpu.VMEM((2, 2, toks, half_piece), bf16),
            dma((5,)),
            dma((12,)),
            dma((2, NCH)),
            dma((NCH, 4)),
            dma((2,)),
            dma((5, NP)),
            dma((2, 2)),
            dma((1,)),
        ],
        compiler_params=pltpu.CompilerParams(
            collective_id=0, has_side_effects=True, vmem_limit_bytes=45_800_000),
    )(tokens, norm_gain.reshape(1, rows), gate_weight, up_weight, down_weight)
    up = lax.ppermute(Tp, "tp", [(i, (i + 1) % RING) for i in range(RING)])
    down = lax.ppermute(Tm, "tp", [(i, (i + RING - 1) % RING) for i in range(RING)])
    g_out, u_out, d_out, half, own = pl.pallas_call(
        write_out,
        out_shape=(
            jax.ShapeDtypeStruct((width, ff), bf16),
            jax.ShapeDtypeStruct((width, ff), bf16),
            jax.ShapeDtypeStruct((ff, width), bf16),
            jax.ShapeDtypeStruct((toks, dcols), bf16),
            pltpu.VMEM((toks, PIECE), f32),
        ),
        in_specs=[vmem] * 4,
        out_specs=(hbm,) * 4 + (vmem,),
        scratch_shapes=[pltpu.VMEM((toks, PIECE), bf16), dma((13,))],
        cost_estimate=pl.CostEstimate(flops=6 * 10**9, bytes_accessed=18 * 10**6, transcendentals=0),
        compiler_params=pltpu.CompilerParams(vmem_limit_bytes=12 * 2**20),
    )(W.reshape(2, width, ff), Dn.reshape(ff, width), H, R1)
    mixed = pl.pallas_call(
        add_last,
        out_shape=jax.ShapeDtypeStruct((toks, dcols), bf16),
        in_specs=[hbm] + [vmem] * 3,
        out_specs=hbm,
        input_output_aliases={0: 0},
        scratch_shapes=[pltpu.VMEM((toks, PIECE), bf16), dma((3,))],
        compiler_params=pltpu.CompilerParams(vmem_limit_bytes=8 * 2**20),
    )(half, own, up, down)
    return g_out, u_out, d_out, mixed


def solution(mesh):
    in_specs = (P("fs", None), P("fs"), P("fs", "tp"), P("fs", "tp"), P("fs", "tp"))
    out_specs = (P(None, "tp"), P(None, "tp"), P("tp", None), P("fs", "tp"))
    return jax.shard_map(
        on_device, mesh=mesh, in_specs=in_specs, out_specs=out_specs, check_vma=False
    )
```
